32 devices in a mesh: fs: 16 (over z, y, core), tp: 2 (over x).
Axes of the slice: x: 2, y: 2, z: 4, core: 2. Of those that a mesh axis runs over, the one named last changes fastest.
Arguments:
- tokens: bfloat16 [4096, 2048], P('fs', 'tp'), may hold values from -16 to 16, as said below
- mix_gain: bfloat16 [2048], P('tp'), may hold values from 0.099609375 to 1.8984375
- query_weight: bfloat16 [2048, 512], P('fs', 'tp'), may hold values from -0.125 to 0.125
- key_weight: bfloat16 [2048, 512], P('fs', 'tp'), may hold values from -0.125 to 0.125
- value_weight: bfloat16 [2048, 1024], P('fs', 'tp'), may hold values from -0.125 to 0.125
- output_gate_weight: bfloat16 [2048, 1024], P('fs', 'tp'), may hold values from -0.125 to 0.125
- out_weight: bfloat16 [1024, 2048], P('tp', 'fs'), may hold values from -0.1875 to 0.1875
- head_rates: float32 [8], P('tp'), may hold values from 0 to 1, as said below
- block_scale: float32 [32], P('fs'), may hold values from 0.5 to 2
- ffn_gain: bfloat16 [2048], P('tp'), may hold values from 0.099609375 to 1.8984375
- ff_gate: bfloat16 [2048, 5632], P('fs', 'tp'), may hold values from -0.125 to 0.125
- ff_up: bfloat16 [2048, 5632], P('fs', 'tp'), may hold values from -0.125 to 0.125
- ff_down: bfloat16 [5632, 2048], P('tp', 'fs'), may hold values from -0.078125 to 0.078125
- final_gain: bfloat16 [2048], P('tp'), may hold values from 0.099609375 to 1.8984375
Outputs:
- layer_out: bfloat16 [4096, 2048], P('fs', 'tp')
The draws below stay inside these ranges and needn't reach their ends.
Inputs may be any that keep to these rules, and one draw needn't show every extreme that they name: `tokens`: column blocks of the activations have different scales. `head_rates`: positive rates.
All inputs are finite; a program needn't handle non-finite values.
Results may differ from the reference program's by a relative error of at most 0.014.
Values may be sent and summed in bfloat16 or wider, within the bound.
No kernel may reach another device: no remote copies, remote signals or barrier semaphores. Data moves between devices by JAX's collectives and lax.ppermute only.
A program may use at most 128 MiB of HBM per device.

```python
import math
import jax
import jax.numpy as jnp
from jax import lax

D = 2048
HEADS = 8
DK = 64
DV = 128
FF = 5632
BLK = 128
SEQ_LEN = 256
TOKENS = 4096
N_TP = 2


def draw_tokens(key, part):
    first, second, third = jax.random.split(jax.random.fold_in(key, 11), 3)
    groups = 2 * N_TP
    scales = jnp.exp(jax.random.uniform(second, (groups,), jnp.float32, -1.2, 1.2))
    base = jnp.clip(jax.random.normal(first, (TOKENS, D), jnp.float32), -4.0, 4.0)
    shaped = base.reshape(TOKENS, groups, D // groups) * scales[None, :, None]
    return shaped.reshape(TOKENS, D).astype(jnp.bfloat16)


def draw_head_rates(key, part):
    first, second, third = jax.random.split(jax.random.fold_in(key, 23), 3)
    fast = jax.random.uniform(first, (HEADS,), jnp.float32, 2.8, 4.3) / BLK
    slow = jax.random.uniform(second, (HEADS,), jnp.float32, 0.3, 1.0) / SEQ_LEN
    order = jax.random.permutation(third, HEADS)
    quick = order < HEADS // 2
    return jnp.where(quick, fast, slow).astype(jnp.float32)


def block_levels(own_key, dims, cuts, low, largest):
    level, own = 1.0, jax.random.fold_in(own_key, 6)
    for dim, parts in cuts:
        heights = jnp.exp(jax.random.uniform(jax.random.fold_in(own, dim), (parts,), jnp.float32, low / len(cuts), largest / len(cuts)))
        level = level * jnp.repeat(heights, dims[dim] // parts).reshape([-1 if axis == dim else 1 for axis in range(len(dims))])
    return level


def noise(rng, extent, scale, limit, shards=(), held_as=jnp.bfloat16):
    drawn = scale * jax.random.normal(rng, extent, jnp.float32)
    if shards:
        drawn = drawn * block_levels(rng, extent, shards, -0.22, 0.18)
    return jnp.clip(drawn, -limit, limit).astype(held_as)


def setup_inputs(seed: int = 0) -> dict:
    seeds = jax.random.split(jax.random.key(seed), 15)
    tokens = draw_tokens(jax.random.fold_in(seeds[14], 71), 0)
    mix_gain = jnp.clip(1.0 + 0.18 * jax.random.normal(seeds[1], (D,), jnp.float32), 0.099609375, 1.8984375).astype(jnp.bfloat16)
    query_weight = noise(seeds[2], (D, HEADS * DK), D ** -0.5, 0.125, ((0, 16), (1, 2)))
    key_weight = noise(seeds[3], (D, HEADS * DK), D ** -0.5, 0.125, ((0, 16), (1, 2)))
    value_weight = noise(seeds[4], (D, HEADS * DV), D ** -0.5, 0.125, ((0, 16), (1, 2)))
    output_gate_weight = noise(seeds[5], (D, HEADS * DV), D ** -0.5, 0.125, ((0, 16), (1, 2)))
    out_weight = noise(seeds[6], (HEADS * DV, D), (HEADS * DV) ** -0.5, 0.1875, ((0, 2), (1, 16)))
    head_rates = draw_head_rates(jax.random.fold_in(seeds[14], 71), 0)
    block_scale = jnp.clip(jnp.exp(math.log(2.0) - 1.3862944 * jax.random.uniform(seeds[8], (TOKENS // BLK,), jnp.float32) ** block_levels(seeds[8], (TOKENS // BLK,), ((0, 16),), -0.2, 0.2)), 0.5, 2.0)
    ffn_gain = jnp.clip(1.0 + 0.18 * jax.random.normal(seeds[9], (D,), jnp.float32), 0.099609375, 1.8984375).astype(jnp.bfloat16)
    ff_gate = noise(seeds[10], (D, FF), D ** -0.5, 0.125, ((0, 16), (1, 2)))
    ff_up = noise(seeds[11], (D, FF), D ** -0.5, 0.125, ((0, 16), (1, 2)))
    ff_down = noise(seeds[12], (FF, D), FF ** -0.5, 0.078125, ((0, 2), (1, 16)))
    final_gain = jnp.clip(1.0 + 0.18 * jax.random.normal(seeds[13], (D,), jnp.float32), 0.099609375, 1.8984375).astype(jnp.bfloat16)
    return dict(tokens=tokens, mix_gain=mix_gain, query_weight=query_weight, key_weight=key_weight, value_weight=value_weight, output_gate_weight=output_gate_weight, out_weight=out_weight, head_rates=head_rates, block_scale=block_scale, ffn_gain=ffn_gain, ff_gate=ff_gate, ff_up=ff_up, ff_down=ff_down, final_gain=final_gain)


EPS = 1e-06
THETA = 10000.0

def rms_norm(values, gain):
    scale = lax.rsqrt(lax.optimization_barrier(jnp.mean(values * values, axis=-1, keepdims=True)) + EPS)
    return values * scale * gain.astype(jnp.float32)

def rotate(values, positions):
    half = values.shape[-1] // 2
    inverse = THETA ** (-jnp.arange(half, dtype=jnp.float32) / half)
    angle = positions.astype(jnp.float32)[:, None] * inverse
    cosine = jnp.cos(angle)[:, None, :]
    sine = jnp.sin(angle)[:, None, :]
    first = values[..., :half]
    second = values[..., half:]
    return jnp.concatenate([first * cosine - second * sine, second * cosine + first * sine], axis=-1)

def retain(query, key, value, rates, scales):
    rows, heads_here, width_k = query.shape
    width_v = value.shape[-1]
    nblk = rows // BLK
    hi = lax.Precision.HIGHEST
    qblk = query.astype(jnp.float32).reshape(nblk, BLK, heads_here, width_k)
    kblk = key.astype(jnp.float32).reshape(nblk, BLK, heads_here, width_k)
    vblk = value.astype(jnp.float32).reshape(nblk, BLK, heads_here, width_v)
    logdec = -rates[None, :] * scales[:, None]
    steps = jnp.arange(BLK, dtype=jnp.float32)
    offset = steps[:, None] - steps[None, :]
    causal = offset >= 0
    inside = jnp.where(causal[None, None], jnp.exp(logdec[:, :, None, None] * jnp.where(causal, offset, 0.0)[None, None]), 0.0)
    scores = jnp.einsum('nchd,nmhd->nhcm', qblk, kblk, precision=hi) * inside
    inner = jnp.einsum('nhcm,nmhe->nche', scores, vblk, precision=hi)
    zeta = jnp.exp(logdec[:, :, None] * (BLK - 1.0 - steps)[None, None, :])
    kv_block = jnp.einsum('nchd,nche->nhde', kblk * jnp.transpose(zeta, (0, 2, 1))[..., None], vblk, precision=hi)
    hold = jnp.exp(logdec * BLK)
    per_seq = SEQ_LEN // BLK
    fresh = (jnp.arange(nblk, dtype=jnp.int32) % per_seq == 0).astype(jnp.float32)

    def advance(state, inputs):
        kv_now, hold_now, fresh_now = inputs
        before = state * (1.0 - fresh_now)
        return (before * hold_now[:, None, None] + kv_now, before)
    start = jnp.zeros((heads_here, width_k, width_v), jnp.float32)
    _, before = lax.scan(advance, start, (kv_block, hold, fresh))
    xi = jnp.exp(logdec[:, :, None] * (steps + 1.0)[None, None, :])
    cross = jnp.einsum('nchd,nhde->nche', qblk * jnp.transpose(xi, (0, 2, 1))[..., None], before, precision=hi)
    total = inner + cross
    total = total * lax.rsqrt(lax.optimization_barrier(jnp.mean(total * total, axis=-1, keepdims=True)) + EPS)
    return total.reshape(rows, heads_here, width_v)

def grouped_product(left, right, groups):
    width = left.shape[1] // groups
    result = jnp.zeros((left.shape[0], right.shape[1]), jnp.float32)
    for index in range(groups):
        partial_sum = jnp.dot(left[:, index * width:(index + 1) * width], right[index * width:(index + 1) * width], preferred_element_type=jnp.float32)
        result = result + partial_sum.astype(jnp.bfloat16).astype(jnp.float32)
    return result

def reference(tokens, mix_gain, query_weight, key_weight, value_weight, output_gate_weight, out_weight, head_rates, block_scale, ffn_gain, ff_gate, ff_up, ff_down, final_gain):
    rows = tokens.shape[0]
    positions = jnp.arange(rows, dtype=jnp.int32) % SEQ_LEN
    normed = rms_norm(tokens.astype(jnp.float32), mix_gain).astype(jnp.bfloat16)
    qproj = jnp.dot(normed, query_weight, preferred_element_type=jnp.float32).reshape(rows, HEADS, DK)
    kproj = jnp.dot(normed, key_weight, preferred_element_type=jnp.float32).reshape(rows, HEADS, DK)
    vproj = jnp.dot(normed, value_weight, preferred_element_type=jnp.float32)
    gproj = jnp.dot(normed, output_gate_weight, preferred_element_type=jnp.float32)
    query = rotate(qproj, positions).astype(jnp.bfloat16)
    key = (rotate(kproj, positions) * DK ** (-0.5)).astype(jnp.bfloat16)
    value = vproj.astype(jnp.bfloat16).reshape(rows, HEADS, DV)
    normret = retain(query, key, value, head_rates, block_scale).reshape(rows, HEADS * DV)
    gated = (normret * jax.nn.silu(gproj)).astype(jnp.bfloat16)
    mix = grouped_product(gated, out_weight, N_TP)
    resid = (tokens.astype(jnp.float32) + mix).astype(jnp.bfloat16)
    normed2 = rms_norm(resid.astype(jnp.float32), ffn_gain).astype(jnp.bfloat16)
    gate_part = jnp.dot(normed2, ff_gate, preferred_element_type=jnp.float32)
    up_part = jnp.dot(normed2, ff_up, preferred_element_type=jnp.float32)
    hidden = (jax.nn.silu(gate_part) * up_part).astype(jnp.bfloat16)
    ffn = grouped_product(hidden, ff_down, N_TP)
    total = resid.astype(jnp.float32) + ffn
    return rms_norm(total, final_gain).astype(jnp.bfloat16)
```

```python
import jax
import jax.numpy as jnp
from jax import lax
from jax.sharding import PartitionSpec as P

DK = 64
DV = 128
BLK = 128
SEQ_LEN = 256
EPS = 1e-06
THETA = 10000.0
F32 = jnp.float32
BF16 = jnp.bfloat16


def factors(fs, heads_here, hidden_here):
    nc = 2 if fs % 2 == 0 and heads_here % 2 == 0 and hidden_here % 256 == 0 else 1
    rest = fs // nc
    ny = max(d for d in range(1, rest + 1) if d**3 <= rest and rest % d == 0)
    return rest // ny, ny, nc


class Grid:
    def __init__(self, heads_here, hidden_here):
        fs = lax.axis_size("fs")
        self.nz, self.ny, self.nc = factors(fs, heads_here, hidden_here)
        nz, ny, nc = self.nz, self.ny, self.nc
        here = lax.axis_index("fs")
        self.c = here % nc
        self.y = (here // nc) % ny
        self.z = here // (nc * ny)
        index = lambda z, y, c: ((z % nz) * ny + y % ny) * nc + c % nc
        every = [(z, y, c) for z in range(nz) for y in range(ny) for c in range(nc)]
        self.to_z = [(index(z, y, c), index(z + 1, y, c)) for z, y, c in every]
        self.to_y = [(index(z, y, c), index(z, y + 1, c)) for z, y, c in every]
        self.to_c = [(index(z, y, c), index(z, y, c + 1)) for z, y, c in every]

    def send_z(self, a):
        return lax.ppermute(a, "fs", self.to_z)

    def send_y(self, a):
        return lax.ppermute(a, "fs", self.to_y)

    def send_c(self, a):
        return lax.ppermute(a, "fs", self.to_c)

    def ring(self, a, send, size):
        pieces = [a]
        for _ in range(size - 1):
            pieces.append(send(pieces[-1]))
        return pieces

    def z_first(self, a):
        return {
            (i, j): piece
            for i, got in enumerate(self.ring(a, self.send_z, self.nz))
            for j, piece in enumerate(self.ring(got, self.send_y, self.ny))
        }

    def y_first(self, a):
        return {
            (i, j): piece
            for j, got in enumerate(self.ring(a, self.send_y, self.ny))
            for i, piece in enumerate(self.ring(got, self.send_z, self.nz))
        }

    def source(self, i, j):
        return ((self.z - i) % self.nz) * self.ny + (self.y - j) % self.ny

    def half(self, a, axis, which):
        if self.nc == 1:
            return a
        low, high = jnp.split(a, 2, axis=axis)
        return jnp.where(which == 0, low, high)

    def join(self, mine, other, axis):
        return jnp.where(
            self.c == 0,
            jnp.concatenate([mine, other], axis=axis),
            jnp.concatenate([other, mine], axis=axis),
        )

    def trade(self, a, split, axis):
        if self.nc == 1:
            return a
        mine = self.half(a, split, self.c)
        other = self.send_c(self.half(a, split, 1 - self.c))
        return self.join(mine, other, axis)

    def both(self, a):
        return a if self.nc == 1 else jnp.concatenate([a, self.send_c(a)], axis=0)

    def reduce_cores(self, a):
        if self.nc == 1:
            return a
        rows = a.shape[0] // 2
        return a[:rows] + self.send_c(a[rows:])


def swap_tp(a):
    return lax.ppermute(a, "tp", [(0, 1), (1, 0)])


def gather_tp(a):
    if lax.axis_size("tp") != 2:
        return lax.all_gather(a, "tp", axis=a.ndim - 1, tiled=True)
    other = swap_tp(a)
    return jnp.where(
        lax.axis_index("tp") == 0,
        jnp.concatenate([a, other], axis=-1),
        jnp.concatenate([other, a], axis=-1),
    )


def scatter_tp(a):
    size = lax.axis_size("tp")
    if size != 2:
        return lax.psum_scatter(a, "tp", scatter_dimension=1, tiled=True).astype(F32)
    low, high = jnp.split(a, 2, axis=1)
    first = lax.axis_index("tp") == 0
    other = swap_tp(jnp.where(first, high, low))
    return jnp.where(first, low, high).astype(F32) + other.astype(F32)


def rms_norm(values, gain):
    scale = lax.rsqrt(jnp.mean(values * values, axis=-1, keepdims=True) + EPS)
    return values * scale * gain.astype(F32)


def rotate(values, positions):
    half = values.shape[-1] // 2
    inverse = THETA ** (-jnp.arange(half, dtype=F32) / half)
    angle = positions.astype(F32)[:, None] * inverse
    cosine = jnp.cos(angle)[:, None, :]
    sine = jnp.sin(angle)[:, None, :]
    first = values[..., :half]
    second = values[..., half:]
    return jnp.concatenate(
        [first * cosine - second * sine, second * cosine + first * sine], axis=-1
    )


def retain(query, key, value, rates, scales):
    rows, heads, width_k = query.shape
    width_v = value.shape[-1]
    per_seq = SEQ_LEN // BLK
    seqs = rows // SEQ_LEN
    hi = lax.Precision.HIGHEST
    qblk = query.reshape(seqs, per_seq, BLK, heads, width_k)
    kblk = key.reshape(seqs, per_seq, BLK, heads, width_k)
    vblk = value.astype(F32).reshape(seqs, per_seq, BLK, heads, width_v)
    logdec = (-rates[None, :] * scales[:, None]).reshape(seqs, per_seq, heads)
    steps = jnp.arange(BLK, dtype=F32)
    offset = steps[:, None] - steps[None, :]
    causal = offset >= 0
    out = []
    for i in range(per_seq):
        ret = 0.0
        for j in range(i + 1):
            here = logdec[:, i, :, None, None]
            if i == j:
                decay = jnp.where(causal, jnp.exp(here * jnp.where(causal, offset, 0.0)), 0.0)
            else:
                power = here * (steps + 1.0)[:, None]
                power += logdec[:, j, :, None, None] * (BLK - 1.0 - steps)[None, :]
                for between in range(j + 1, i):
                    power += logdec[:, between, :, None, None] * BLK
                decay = jnp.exp(power)
            scores = jnp.einsum(
                "schd,smhd->shcm", qblk[:, i], kblk[:, j], preferred_element_type=F32
            )
            ret += jnp.einsum("shcm,smhe->sche", scores * decay, vblk[:, j], precision=hi)
        out.append(ret)
    total = jnp.stack(out, axis=1)
    total = total * lax.rsqrt(jnp.mean(total * total, axis=-1, keepdims=True) + EPS)
    return total.reshape(rows, heads * width_v)


def body(
    tokens,
    mix_gain,
    query_weight,
    key_weight,
    value_weight,
    output_gate_weight,
    out_weight,
    head_rates,
    block_scale,
    ffn_gain,
    ff_gate,
    ff_up,
    ff_down,
    final_gain,
):
    heads_here = head_rates.shape[0]
    grid = Grid(heads_here, ff_up.shape[1])
    heads = heads_here // grid.nc
    dot = lambda a, b: jnp.dot(a, b, preferred_element_type=F32)

    in_proj = [
        grid.half(w, 1, grid.c) for w in (query_weight, key_weight, value_weight, output_gate_weight)
    ]
    in_proj = jnp.concatenate(in_proj, axis=1)
    if grid.nc == 2:
        away = [
            grid.half(w, 1, 1 - grid.c)
            for w in (query_weight, key_weight, value_weight, output_gate_weight)
        ]
        in_proj = grid.join(in_proj, grid.send_c(jnp.concatenate(away, axis=1)), 0)
    in_pieces = grid.y_first(in_proj)
    out_pieces = grid.y_first(grid.trade(out_weight, 0, 1))
    gate_pieces = grid.z_first(grid.trade(ff_gate, 1, 0))
    up_pieces = grid.z_first(grid.trade(ff_up, 1, 0))
    down_pieces = grid.z_first(grid.trade(ff_down, 0, 1))

    chips = grid.nz * grid.ny

    def by_chip(a):
        return jnp.transpose(a.reshape(a.shape[0], chips, a.shape[1] // chips), (1, 0, 2))

    def contract(blocks, pieces):
        return sum(
            dot(lax.dynamic_index_in_dim(blocks, grid.source(*at), keepdims=False), piece)
            for at, piece in pieces.items()
        )

    def expand(a, pieces):
        width = next(iter(pieces.values())).shape[1]
        rows = a.shape[0] // grid.nc
        out = jnp.zeros((chips, rows, width), BF16)
        for at, piece in pieces.items():
            part = grid.reduce_cores(dot(a, piece)).astype(BF16)
            out = lax.dynamic_update_index_in_dim(out, part, grid.source(*at), 0)
        return jnp.transpose(out, (1, 0, 2)).reshape(rows, chips * width)

    whole = gather_tp(tokens)
    normed = rms_norm(whole.astype(F32), gather_tp(mix_gain)).astype(BF16)
    normed = grid.both(normed)
    rows = normed.shape[0]
    positions = jnp.arange(rows, dtype=jnp.int32) % SEQ_LEN
    proj = contract(by_chip(normed), in_pieces)
    k_at, v_at, g_at = heads * DK, 2 * heads * DK, 2 * heads * DK + heads * DV
    qproj, kproj, vproj, gproj = jnp.split(proj, (k_at, v_at, g_at), axis=1)
    query = rotate(qproj.reshape(rows, heads, DK), positions).astype(BF16)
    key = (rotate(kproj.reshape(rows, heads, DK), positions) * DK ** (-0.5)).astype(BF16)
    value = vproj.astype(BF16).reshape(rows, heads, DV)
    rates = grid.half(head_rates, 0, grid.c)
    normret = retain(query, key, value, rates, grid.both(block_scale))
    gated = (normret * jax.nn.silu(gproj)).astype(BF16)
    mix = scatter_tp(expand(gated, out_pieces))
    resid = (tokens.astype(F32) + mix).astype(BF16)

    whole2 = gather_tp(resid)
    normed2 = rms_norm(whole2.astype(F32), gather_tp(ffn_gain)).astype(BF16)
    blocks2 = by_chip(grid.both(normed2))
    gate_part = contract(blocks2, gate_pieces)
    up_part = contract(blocks2, up_pieces)
    hidden = (jax.nn.silu(gate_part) * up_part).astype(BF16)
    ffn = scatter_tp(expand(hidden, down_pieces))
    total = resid.astype(F32) + ffn
    features = tokens.shape[1] * lax.axis_size("tp")
    squares = lax.psum(jnp.sum(total * total, axis=-1, keepdims=True), "tp")
    scale = lax.rsqrt(squares / features + EPS)
    return (total * scale * final_gain.astype(F32)).astype(BF16)


def solution(mesh):
    return jax.shard_map(
        body,
        mesh=mesh,
        in_specs=(
            P("fs", "tp"),
            P("tp"),
            P("fs", "tp"),
            P("fs", "tp"),
            P("fs", "tp"),
            P("fs", "tp"),
            P("tp", "fs"),
            P("tp"),
            P("fs"),
            P("tp"),
            P("fs", "tp"),
            P("fs", "tp"),
            P("tp", "fs"),
            P("tp"),
        ),
        out_specs=P("fs", "tp"),
        check_vma=False,
    )
```

```python
import jax
import jax.numpy as jnp
from jax import lax
from jax.sharding import PartitionSpec as P

D = 2048
DK = 64
DV = 128
BLK = 128
SEQ_LEN = 256
EPS = 1e-06
THETA = 10000.0
F32 = jnp.float32
BF16 = jnp.bfloat16


def rms_norm(values, gain):
    scale = lax.rsqrt(jnp.mean(values * values, axis=-1, keepdims=True) + EPS)
    return values * scale * gain.astype(jnp.float32)


def rotate(values, positions):
    half = values.shape[-1] // 2
    inverse = THETA ** (-jnp.arange(half, dtype=jnp.float32) / half)
    angle = positions.astype(jnp.float32)[:, None] * inverse
    cosine = jnp.cos(angle)[:, None, :]
    sine = jnp.sin(angle)[:, None, :]
    first = values[..., :half]
    second = values[..., half:]
    return jnp.concatenate(
        [first * cosine - second * sine, second * cosine + first * sine], axis=-1
    )


def plain_retain(query, key, value, rates, scales):
    rows, heads_here, width_k = query.shape
    width_v = value.shape[-1]
    nblk = rows // BLK
    hi = lax.Precision.HIGHEST
    qblk = query.astype(jnp.float32).reshape(nblk, BLK, heads_here, width_k)
    kblk = key.astype(jnp.float32).reshape(nblk, BLK, heads_here, width_k)
    vblk = value.astype(jnp.float32).reshape(nblk, BLK, heads_here, width_v)
    logdec = -rates[None, :] * scales[:, None]
    steps = jnp.arange(BLK, dtype=jnp.float32)
    offset = steps[:, None] - steps[None, :]
    causal = offset >= 0
    inside = jnp.where(
        causal[None, None],
        jnp.exp(logdec[:, :, None, None] * jnp.where(causal, offset, 0.0)[None, None]),
        0.0,
    )
    scores = jnp.einsum("nchd,nmhd->nhcm", qblk, kblk, precision=hi) * inside
    inner = jnp.einsum("nhcm,nmhe->nche", scores, vblk, precision=hi)
    zeta = jnp.exp(logdec[:, :, None] * (BLK - 1.0 - steps)[None, None, :])
    kv_block = jnp.einsum(
        "nchd,nche->nhde", kblk * jnp.transpose(zeta, (0, 2, 1))[..., None], vblk, precision=hi
    )
    hold = jnp.exp(logdec * BLK)
    per_seq = SEQ_LEN // BLK
    fresh = (jnp.arange(nblk, dtype=jnp.int32) % per_seq == 0).astype(jnp.float32)

    def advance(state, inputs):
        kv_now, hold_now, fresh_now = inputs
        before = state * (1.0 - fresh_now)
        return (before * hold_now[:, None, None] + kv_now, before)

    start = jnp.zeros((heads_here, width_k, width_v), jnp.float32)
    _, before = lax.scan(advance, start, (kv_block, hold, fresh))
    xi = jnp.exp(logdec[:, :, None] * (steps + 1.0)[None, None, :])
    cross = jnp.einsum(
        "nchd,nhde->nche", qblk * jnp.transpose(xi, (0, 2, 1))[..., None], before, precision=hi
    )
    total = inner + cross
    total = total * lax.rsqrt(jnp.mean(total * total, axis=-1, keepdims=True) + EPS)
    return total.reshape(rows, heads_here * width_v)


def fold_maker(source, pieces):
    return tuple((jnp.dot(source, piece, preferred_element_type=jnp.float32) for piece in pieces))


def plain_body(
    tokens,
    mix_gain,
    query_weight,
    key_weight,
    value_weight,
    output_gate_weight,
    out_weight,
    head_rates,
    block_scale,
    ffn_gain,
    ff_gate,
    ff_up,
    ff_down,
    final_gain,
):
    rows = tokens.shape[0]
    heads_here = head_rates.shape[0]
    groups = lax.axis_size("tp")
    positions = jnp.arange(rows, dtype=jnp.int32) % SEQ_LEN
    whole, gain_whole = (
        lax.all_gather(tokens, "tp", axis=1, tiled=True),
        lax.all_gather(mix_gain, "tp", axis=0, tiled=True),
    )
    normed = rms_norm(whole.astype(jnp.float32), gain_whole).astype(jnp.bfloat16)
    qproj, kproj, vproj, gproj = fold_maker(
        normed,
        (
            lax.all_gather(query_weight, "fs", axis=0, tiled=True),
            lax.all_gather(key_weight, "fs", axis=0, tiled=True),
            lax.all_gather(value_weight, "fs", axis=0, tiled=True),
            lax.all_gather(output_gate_weight, "fs", axis=0, tiled=True),
        ),
    )
    query = rotate(qproj.reshape(rows, heads_here, DK), positions).astype(jnp.bfloat16)
    key = (rotate(kproj.reshape(rows, heads_here, DK), positions) * DK ** (-0.5)).astype(
        jnp.bfloat16
    )
    value = vproj.astype(jnp.bfloat16).reshape(rows, heads_here, DV)
    normret = plain_retain(query, key, value, head_rates, block_scale)
    gated = (normret * jax.nn.silu(gproj)).astype(jnp.bfloat16)
    all_heads = lax.all_gather(gated, "tp", axis=1, tiled=True)
    head_rows = lax.all_gather(out_weight, "fs", axis=1, tiled=True)
    feature_block = lax.all_to_all(head_rows, "tp", split_axis=1, concat_axis=0, tiled=True)
    width = all_heads.shape[1] // groups
    left = all_heads.reshape(rows, groups, width)
    right = feature_block.reshape(groups, width, feature_block.shape[1])
    partial_sums = jnp.einsum(
        "rng,nge->nre", left, right, preferred_element_type=jnp.float32
    ).astype(jnp.bfloat16)
    mix = jnp.sum(partial_sums.astype(jnp.float32), axis=0)
    resid = (tokens.astype(jnp.float32) + mix).astype(jnp.bfloat16)
    whole2, gain2 = (
        lax.all_gather(resid, "tp", axis=1, tiled=True),
        lax.all_gather(ffn_gain, "tp", axis=0, tiled=True),
    )
    normed2 = rms_norm(whole2.astype(jnp.float32), gain2).astype(jnp.bfloat16)
    gate_part, up_part = fold_maker(
        normed2,
        (
            lax.all_gather(ff_gate, "fs", axis=0, tiled=True),
            lax.all_gather(ff_up, "fs", axis=0, tiled=True),
        ),
    )
    hidden = (jax.nn.silu(gate_part) * up_part).astype(jnp.bfloat16)
    down_terms = jnp.dot(
        hidden,
        lax.all_gather(ff_down, "fs", axis=1, tiled=True),
        preferred_element_type=jnp.float32,
    )
    ffn = lax.psum_scatter(
        down_terms.astype(jnp.bfloat16), "tp", scatter_dimension=1, tiled=True
    ).astype(jnp.float32)
    total = resid.astype(jnp.float32) + ffn
    squares = lax.psum(jnp.sum(total * total, axis=-1, keepdims=True), "tp")
    scale = lax.rsqrt(squares / D + EPS)
    return (total * scale * final_gain.astype(jnp.float32)).astype(jnp.bfloat16)


class Group:
    def __init__(self):
        self.nz = lax.axis_size("fs") // 4
        here = lax.axis_index("fs")
        self.c = here % 2
        self.y = (here // 2) % 2
        self.z = here // 4
        every = range(4 * self.nz)
        self.to_c = [(i, i ^ 1) for i in every]
        self.to_y = [(i, i ^ 2) for i in every]
        self.to_z = [(i, (i + 4) % (4 * self.nz)) for i in every]

    def send(self, a, to):
        return lax.ppermute(a, "fs", to)

    def swap_c(self, a):
        return self.send(a, self.to_c)

    def swap_y(self, a):
        return self.send(a, self.to_y)

    def trade(self, parts, axis):
        low = parts[:, 0]
        high = parts[:, 1]
        first = self.c == 0
        mine = jnp.where(first, low, high)
        other = self.swap_c(jnp.where(first, high, low))
        joined = jnp.where(
            first,
            jnp.concatenate([mine, other], axis=axis + 1),
            jnp.concatenate([other, mine], axis=axis + 1),
        )
        near = self.y == 0
        own = jnp.where(near, joined[0], joined[1])
        return own, self.swap_y(jnp.where(near, joined[1], joined[0]))

    def ring(self, a):
        pieces = [a]
        for _ in range(1, self.nz):
            pieces.append(self.send(pieces[-1], self.to_z))
        return pieces

    def by_y(self, own, other):
        near = self.y == 0
        return jnp.where(near, own, other), jnp.where(near, other, own)

    def block(self, i, far):
        return ((self.z - i) % self.nz) * 2 + (self.y ^ far)

    def assemble(self, own, other):
        out = jnp.zeros((2 * self.nz, *own[0].shape), own[0].dtype)
        for i in range(self.nz):
            out = lax.dynamic_update_index_in_dim(out, own[i], self.block(i, 0), 0)
            out = lax.dynamic_update_index_in_dim(out, other[i], self.block(i, 1), 0)
        return out

    def gather_rows(self, a):
        pair = jnp.concatenate([a, self.swap_y(a)], axis=0)
        return jnp.concatenate([pair, self.swap_c(pair)], axis=0)

    def scatter_rows(self, a):
        rows = a.shape[0] // 2
        pair = a[:rows] + self.swap_c(a[rows:].astype(BF16)).astype(F32)
        rows //= 2
        return pair[:rows] + self.swap_y(pair[rows:].astype(BF16)).astype(F32)


def swap_x(a):
    return lax.ppermute(a, "tp", [(0, 1), (1, 0)])


def join_x(a):
    other = swap_x(a)
    return jnp.where(
        lax.axis_index("tp") == 0,
        jnp.concatenate([a, other], axis=-1),
        jnp.concatenate([other, a], axis=-1),
    )


def sum_x(a):
    mine = a.astype(BF16)
    return mine.astype(F32) + swap_x(mine).astype(F32)


def retain(query, key, value, rates, scales):
    rows, heads, width_k = query.shape
    width_v = value.shape[-1]
    per_seq = SEQ_LEN // BLK
    seqs = rows // SEQ_LEN
    hi = lax.Precision.HIGHEST
    qblk = query.reshape(seqs, per_seq, BLK, heads, width_k)
    kblk = key.reshape(seqs, per_seq, BLK, heads, width_k)
    vblk = value.astype(F32).reshape(seqs, per_seq, BLK, heads, width_v)
    logdec = (-rates[None, :] * scales[:, None]).reshape(seqs, per_seq, heads)
    steps = jnp.arange(BLK, dtype=F32)
    offset = steps[:, None] - steps[None, :]
    causal = offset >= 0
    out = []
    for i in range(per_seq):
        ret = 0.0
        here = logdec[:, i, :, None, None]
        for j in range(i + 1):
            if i == j:
                decay = jnp.where(causal, jnp.exp(here * jnp.where(causal, offset, 0.0)), 0.0)
            else:
                power = here * (steps + 1.0)[:, None]
                power += logdec[:, j, :, None, None] * (BLK - 1.0 - steps)[None, :]
                for between in range(j + 1, i):
                    power += logdec[:, between, :, None, None] * BLK
                decay = jnp.exp(power)
            scores = jnp.einsum(
                "schd,smhd->shcm", qblk[:, i], kblk[:, j], preferred_element_type=F32
            )
            ret += jnp.einsum("shcm,smhe->sche", scores * decay, vblk[:, j], precision=hi)
        out.append(ret)
    total = jnp.stack(out, axis=1)
    total = total * lax.rsqrt(jnp.mean(total * total, axis=-1, keepdims=True) + EPS)
    return total.reshape(rows, heads * width_v)


def group_body(
    tokens,
    mix_gain,
    query_weight,
    key_weight,
    value_weight,
    output_gate_weight,
    out_weight,
    head_rates,
    block_scale,
    ffn_gain,
    ff_gate,
    ff_up,
    ff_down,
    final_gain,
):
    group = Group()
    nz = group.nz
    x = lax.axis_index("tp")
    heads = head_rates.shape[0] // 4
    dot = lambda a, b: jnp.dot(a, b, preferred_element_type=F32)

    def columns(*weights):
        quarters = [jnp.split(w, 4, axis=1) for w in weights]
        parts = jnp.stack([jnp.concatenate(q, axis=1) for q in zip(*quarters, strict=True)])
        return parts.reshape(2, 2, *parts.shape[1:])

    def rows_of(w):
        return w.reshape(2, 2, w.shape[0] // 4, w.shape[1])

    whole = join_x(tokens)
    in_own, in_other = group.trade(
        columns(query_weight, key_weight, value_weight, output_gate_weight), 0
    )
    in_own, out_weight, ff_gate, ff_up, ff_down, mix_gain, block_scale = lax.optimization_barrier(
        (in_own, out_weight, ff_gate, ff_up, ff_down, mix_gain, block_scale)
    )
    out_pair = group.trade(rows_of(out_weight), 1)
    in_pieces = group.ring(in_own), group.ring(in_other)
    out_pieces = group.ring(jnp.stack(out_pair))
    gains = join_x(jnp.stack([mix_gain, ffn_gain]))
    scales = group.gather_rows(block_scale)
    up_own, up_other = group.trade(columns(ff_gate, ff_up), 0)
    down = group.by_y(*group.trade(rows_of(ff_down), 1))
    upa, upb = [up_own], [up_other]
    down0, down1 = [down[0]], [down[1]]

    def step(pieces, *after):
        piece = pieces[-1]
        if after:
            piece, *_ = lax.optimization_barrier((piece, *after))
        pieces.append(group.send(piece, group.to_z))

    step(upa)

    normed = rms_norm(whole.astype(F32), gains[0]).astype(BF16)
    normed = group.gather_rows(normed)
    rows = normed.shape[0]
    positions = jnp.arange(rows, dtype=jnp.int32) % SEQ_LEN
    in_full = group.assemble(*in_pieces)
    proj = dot(normed, in_full.reshape(normed.shape[1], -1))
    step(upb, proj)
    step(down0, proj)
    k_at, v_at, g_at = heads * DK, 2 * heads * DK, 2 * heads * DK + heads * DV
    qproj, kproj, vproj, gproj = jnp.split(proj, (k_at, v_at, g_at), axis=1)
    query = rotate(qproj.reshape(rows, heads, DK), positions).astype(BF16)
    key = (rotate(kproj.reshape(rows, heads, DK), positions) * DK ** (-0.5)).astype(BF16)
    value = vproj.astype(BF16).reshape(rows, heads, DV)
    rates = lax.dynamic_slice_in_dim(head_rates, (group.y * 2 + group.c) * heads, heads)
    normret = retain(query, key, value, rates, scales)
    gated = (normret * jax.nn.silu(gproj)).astype(BF16)
    step(upa, gated)
    step(upb, gated)
    step(down1, gated)
    for _ in range(2, nz):
        step(upa)
        step(upb)

    out_full = group.assemble([p[0] for p in out_pieces], [p[1] for p in out_pieces])
    out_full = jnp.transpose(out_full, (1, 0, 2)).reshape(out_full.shape[1], -1)
    resid = []
    for w, t in zip(jnp.split(out_full, 2, axis=1), jnp.split(whole, 2, axis=1), strict=True):
        part = group.scatter_rows(dot(gated, w))
        resid.append((t.astype(F32) + sum_x(part)).astype(BF16))
    resid = jnp.concatenate(resid, axis=1)
    normed2 = rms_norm(resid.astype(F32), gains[1]).astype(BF16)
    normed2 = group.gather_rows(normed2)

    for _ in range(2, nz):
        step(down0)
        step(down1)
    up_full = group.assemble(upa, upb)
    both = dot(normed2, up_full.reshape(normed2.shape[1], -1))
    gate_part, up_part = jnp.split(both, 2, axis=1)
    hidden = (jax.nn.silu(gate_part) * up_part).astype(BF16)

    resid = jnp.transpose(resid.reshape(resid.shape[0], nz, -1), (1, 0, 2))
    total = []
    squares = 0.0
    for i in range(nz):
        weight = jnp.concatenate([down0[i], down1[i]], axis=1)
        part = group.scatter_rows(dot(hidden, weight))
        now = lax.dynamic_index_in_dim(resid, (group.z - i) % nz, keepdims=False).astype(F32)
        now = now + sum_x(part)
        squares += jnp.sum(now * now, axis=-1, keepdims=True)
        total.append(now)
    scale = lax.rsqrt(squares / (tokens.shape[1] * lax.axis_size("tp")) + EPS)
    mine = [
        lax.select_n((group.z - (x * (nz // 2) + k)) % nz, *total) for k in range(nz // 2)
    ]
    return (jnp.concatenate(mine, axis=1) * scale * final_gain.astype(F32)).astype(BF16)


def grouped(fs, tp, heads_here, hidden_here):
    split = fs % 4 == 0 and heads_here % 4 == 0 and hidden_here % 64 == 0
    return split and tp == 2 and fs // 4 == 4


def solution(mesh):
    fs, tp = mesh.shape["fs"], mesh.shape["tp"]

    def body(*args):
        if not grouped(fs, tp, args[7].shape[0], args[10].shape[1]):
            return plain_body(*args)
        return group_body(*args)

    return jax.shard_map(
        body,
        mesh=mesh,
        in_specs=(
            P("fs", "tp"),
            P("tp"),
            P("fs", "tp"),
            P("fs", "tp"),
            P("fs", "tp"),
            P("fs", "tp"),
            P("tp", "fs"),
            P("tp"),
            P("fs"),
            P("tp"),
            P("fs", "tp"),
            P("fs", "tp"),
            P("tp", "fs"),
            P("tp"),
        ),
        out_specs=P("fs", "tp"),
        check_vma=False,
    )
```

```python
import jax
import jax.numpy as jnp
from jax import lax
from jax.sharding import PartitionSpec as P

D = 2048
DK = 64
DV = 128
BLK = 128
SEQ_LEN = 256
EPS = 1e-06
THETA = 10000.0
F32 = jnp.float32
BF16 = jnp.bfloat16


def rms_norm(values, gain):
    scale = lax.rsqrt(jnp.mean(values * values, axis=-1, keepdims=True) + EPS)
    return values * scale * gain.astype(jnp.float32)


def rotate(values, positions):
    half = values.shape[-1] // 2
    inverse = THETA ** (-jnp.arange(half, dtype=jnp.float32) / half)
    angle = positions.astype(jnp.float32)[:, None] * inverse
    cosine = jnp.cos(angle)[:, None, :]
    sine = jnp.sin(angle)[:, None, :]
    first = values[..., :half]
    second = values[..., half:]
    return jnp.concatenate(
        [first * cosine - second * sine, second * cosine + first * sine], axis=-1
    )


def plain_retain(query, key, value, rates, scales):
    rows, heads_here, width_k = query.shape
    width_v = value.shape[-1]
    nblk = rows // BLK
    hi = lax.Precision.HIGHEST
    qblk = query.astype(jnp.float32).reshape(nblk, BLK, heads_here, width_k)
    kblk = key.astype(jnp.float32).reshape(nblk, BLK, heads_here, width_k)
    vblk = value.astype(jnp.float32).reshape(nblk, BLK, heads_here, width_v)
    logdec = -rates[None, :] * scales[:, None]
    steps = jnp.arange(BLK, dtype=jnp.float32)
    offset = steps[:, None] - steps[None, :]
    causal = offset >= 0
    inside = jnp.where(
        causal[None, None],
        jnp.exp(logdec[:, :, None, None] * jnp.where(causal, offset, 0.0)[None, None]),
        0.0,
    )
    scores = jnp.einsum("nchd,nmhd->nhcm", qblk, kblk, precision=hi) * inside
    inner = jnp.einsum("nhcm,nmhe->nche", scores, vblk, precision=hi)
    zeta = jnp.exp(logdec[:, :, None] * (BLK - 1.0 - steps)[None, None, :])
    kv_block = jnp.einsum(
        "nchd,nche->nhde", kblk * jnp.transpose(zeta, (0, 2, 1))[..., None], vblk, precision=hi
    )
    hold = jnp.exp(logdec * BLK)
    per_seq = SEQ_LEN // BLK
    fresh = (jnp.arange(nblk, dtype=jnp.int32) % per_seq == 0).astype(jnp.float32)

    def advance(state, inputs):
        kv_now, hold_now, fresh_now = inputs
        before = state * (1.0 - fresh_now)
        return (before * hold_now[:, None, None] + kv_now, before)

    start = jnp.zeros((heads_here, width_k, width_v), jnp.float32)
    _, before = lax.scan(advance, start, (kv_block, hold, fresh))
    xi = jnp.exp(logdec[:, :, None] * (steps + 1.0)[None, None, :])
    cross = jnp.einsum(
        "nchd,nhde->nche", qblk * jnp.transpose(xi, (0, 2, 1))[..., None], before, precision=hi
    )
    total = inner + cross
    total = total * lax.rsqrt(jnp.mean(total * total, axis=-1, keepdims=True) + EPS)
    return total.reshape(rows, heads_here * width_v)


def fold_maker(source, pieces):
    return tuple((jnp.dot(source, piece, preferred_element_type=jnp.float32) for piece in pieces))


def plain_body(
    tokens,
    mix_gain,
    query_weight,
    key_weight,
    value_weight,
    output_gate_weight,
    out_weight,
    head_rates,
    block_scale,
    ffn_gain,
    ff_gate,
    ff_up,
    ff_down,
    final_gain,
):
    rows = tokens.shape[0]
    heads_here = head_rates.shape[0]
    groups = lax.axis_size("tp")
    positions = jnp.arange(rows, dtype=jnp.int32) % SEQ_LEN
    whole, gain_whole = (
        lax.all_gather(tokens, "tp", axis=1, tiled=True),
        lax.all_gather(mix_gain, "tp", axis=0, tiled=True),
    )
    normed = rms_norm(whole.astype(jnp.float32), gain_whole).astype(jnp.bfloat16)
    qproj, kproj, vproj, gproj = fold_maker(
        normed,
        (
            lax.all_gather(query_weight, "fs", axis=0, tiled=True),
            lax.all_gather(key_weight, "fs", axis=0, tiled=True),
            lax.all_gather(value_weight, "fs", axis=0, tiled=True),
            lax.all_gather(output_gate_weight, "fs", axis=0, tiled=True),
        ),
    )
    query = rotate(qproj.reshape(rows, heads_here, DK), positions).astype(jnp.bfloat16)
    key = (rotate(kproj.reshape(rows, heads_here, DK), positions) * DK ** (-0.5)).astype(
        jnp.bfloat16
    )
    value = vproj.astype(jnp.bfloat16).reshape(rows, heads_here, DV)
    normret = plain_retain(query, key, value, head_rates, block_scale)
    gated = (normret * jax.nn.silu(gproj)).astype(jnp.bfloat16)
    all_heads = lax.all_gather(gated, "tp", axis=1, tiled=True)
    head_rows = lax.all_gather(out_weight, "fs", axis=1, tiled=True)
    feature_block = lax.all_to_all(head_rows, "tp", split_axis=1, concat_axis=0, tiled=True)
    width = all_heads.shape[1] // groups
    left = all_heads.reshape(rows, groups, width)
    right = feature_block.reshape(groups, width, feature_block.shape[1])
    partial_sums = jnp.einsum(
        "rng,nge->nre", left, right, preferred_element_type=jnp.float32
    ).astype(jnp.bfloat16)
    mix = jnp.sum(partial_sums.astype(jnp.float32), axis=0)
    resid = (tokens.astype(jnp.float32) + mix).astype(jnp.bfloat16)
    whole2, gain2 = (
        lax.all_gather(resid, "tp", axis=1, tiled=True),
        lax.all_gather(ffn_gain, "tp", axis=0, tiled=True),
    )
    normed2 = rms_norm(whole2.astype(jnp.float32), gain2).astype(jnp.bfloat16)
    gate_part, up_part = fold_maker(
        normed2,
        (
            lax.all_gather(ff_gate, "fs", axis=0, tiled=True),
            lax.all_gather(ff_up, "fs", axis=0, tiled=True),
        ),
    )
    hidden = (jax.nn.silu(gate_part) * up_part).astype(jnp.bfloat16)
    down_terms = jnp.dot(
        hidden,
        lax.all_gather(ff_down, "fs", axis=1, tiled=True),
        preferred_element_type=jnp.float32,
    )
    ffn = lax.psum_scatter(
        down_terms.astype(jnp.bfloat16), "tp", scatter_dimension=1, tiled=True
    ).astype(jnp.float32)
    total = resid.astype(jnp.float32) + ffn
    squares = lax.psum(jnp.sum(total * total, axis=-1, keepdims=True), "tp")
    scale = lax.rsqrt(squares / D + EPS)
    return (total * scale * final_gain.astype(jnp.float32)).astype(jnp.bfloat16)


class Group:
    def __init__(self):
        self.nz = lax.axis_size("fs") // 4
        here = lax.axis_index("fs")
        self.c = here % 2
        self.y = (here // 2) % 2
        self.z = here // 4
        every = range(4 * self.nz)
        self.to_c = [(i, i ^ 1) for i in every]
        self.to_y = [(i, i ^ 2) for i in every]
        self.to_z = [(i, (i + 4) % (4 * self.nz)) for i in every]

    def send(self, a, to):
        return lax.ppermute(a, "fs", to)

    def swap_c(self, a):
        return self.send(a, self.to_c)

    def swap_y(self, a):
        return self.send(a, self.to_y)

    def trade(self, parts, axis):
        low = parts[:, 0]
        high = parts[:, 1]
        first = self.c == 0
        mine = jnp.where(first, low, high)
        other = self.swap_c(jnp.where(first, high, low))
        joined = jnp.where(
            first,
            jnp.concatenate([mine, other], axis=axis + 1),
            jnp.concatenate([other, mine], axis=axis + 1),
        )
        near = self.y == 0
        own = jnp.where(near, joined[0], joined[1])
        return own, self.swap_y(jnp.where(near, joined[1], joined[0]))

    def ring(self, a):
        pieces = [a]
        for _ in range(1, self.nz):
            pieces.append(self.send(pieces[-1], self.to_z))
        return pieces

    def by_y(self, own, other, axis):
        return jnp.where(
            self.y == 0,
            jnp.concatenate([own, other], axis=axis),
            jnp.concatenate([other, own], axis=axis),
        )

    def turn(self, a):
        parts = jnp.split(a, self.nz, axis=-1)
        orders = [
            jnp.concatenate([parts[(z - i) % self.nz] for i in range(self.nz)], axis=-1)
            for z in range(self.nz)
        ]
        return lax.select_n(self.z, *orders)

    def assemble(self, own, other, after):
        first = jnp.zeros((), own[0].dtype), own[0], other[0]
        (zero, *first), _ = lax.optimization_barrier((first, after))
        own, other = [first[0], *own[1:]], [first[1], *other[1:]]
        out = jnp.broadcast_to(zero, (2 * self.nz, *own[0].shape))
        for i in range(self.nz):
            out = lax.dynamic_update_index_in_dim(out, own[i], 2 * i + self.y, 0)
            out = lax.dynamic_update_index_in_dim(out, other[i], 2 * i + 1 - self.y, 0)
        return out.reshape(-1, out.shape[-1])

    def gather_rows(self, a):
        pair = jnp.concatenate([a, self.swap_y(a)], axis=0)
        return jnp.concatenate([pair, self.swap_c(pair)], axis=0)

    def scatter_pair(self, a, b):
        pair = a + self.swap_c(b.astype(BF16)).astype(F32)
        rows = a.shape[0] // 2
        return pair[:rows] + self.swap_y(pair[rows:].astype(BF16)).astype(F32)


def swap_x(a):
    return lax.ppermute(a, "tp", [(0, 1), (1, 0)])


def join_x(a):
    other = swap_x(a)
    return jnp.where(
        lax.axis_index("tp") == 0,
        jnp.concatenate([a, other], axis=-1),
        jnp.concatenate([other, a], axis=-1),
    )


def sum_x(a):
    mine = a.astype(BF16)
    return mine.astype(F32) + swap_x(mine).astype(F32)


def retain(query, key, value, rates, scales):
    rows, heads, width_k = query.shape
    width_v = value.shape[-1]
    per_seq = SEQ_LEN // BLK
    seqs = rows // SEQ_LEN
    hi = lax.Precision.HIGHEST
    qblk = query.reshape(seqs, per_seq, BLK, heads, width_k)
    kblk = key.reshape(seqs, per_seq, BLK, heads, width_k)
    vblk = value.astype(F32).reshape(seqs, per_seq, BLK, heads, width_v)
    logdec = (-rates[None, :] * scales[:, None]).reshape(seqs, per_seq, heads)
    steps = jnp.arange(BLK, dtype=F32)
    offset = steps[:, None] - steps[None, :]
    causal = offset >= 0
    out = []
    for i in range(per_seq):
        ret = 0.0
        here = logdec[:, i, :, None, None]
        for j in range(i + 1):
            if i == j:
                decay = jnp.where(causal, jnp.exp(here * jnp.where(causal, offset, 0.0)), 0.0)
            else:
                power = here * (steps + 1.0)[:, None]
                power += logdec[:, j, :, None, None] * (BLK - 1.0 - steps)[None, :]
                for between in range(j + 1, i):
                    power += logdec[:, between, :, None, None] * BLK
                decay = jnp.exp(power)
            scores = jnp.einsum(
                "schd,smhd->shcm", qblk[:, i], kblk[:, j], preferred_element_type=F32
            )
            ret += jnp.einsum("shcm,smhe->sche", scores * decay, vblk[:, j], precision=hi)
        out.append(ret)
    total = jnp.stack(out, axis=1)
    total = total * lax.rsqrt(jnp.mean(total * total, axis=-1, keepdims=True) + EPS)
    return total.reshape(rows, heads * width_v)


def group_body(
    tokens,
    mix_gain,
    query_weight,
    key_weight,
    value_weight,
    output_gate_weight,
    out_weight,
    head_rates,
    block_scale,
    ffn_gain,
    ff_gate,
    ff_up,
    ff_down,
    final_gain,
):
    group = Group()
    nz = group.nz
    x = lax.axis_index("tp")
    heads = head_rates.shape[0] // 4
    dot = lambda a, b: jnp.dot(a, b, preferred_element_type=F32)

    def columns(*weights):
        quarters = [jnp.split(w, 4, axis=1) for w in weights]
        parts = jnp.stack([jnp.concatenate(q, axis=1) for q in zip(*quarters, strict=True)])
        return parts.reshape(2, 2, *parts.shape[1:])

    def rows_of(w):
        return w.reshape(2, 2, w.shape[0] // 4, w.shape[1])

    gain = group.turn(join_x(mix_gain))
    whole = group.turn(join_x(tokens))
    in_own, in_other = group.trade(
        columns(query_weight, key_weight, value_weight, output_gate_weight), 0
    )
    out_pair = group.trade(rows_of(out_weight), 1)
    down_own, down_other = group.trade(rows_of(ff_down), 1)
    in_own, ff_gate, ff_up = lax.optimization_barrier((in_own, ff_gate, ff_up))
    in_pieces = zip(group.ring(in_own), group.ring(in_other), strict=True)
    in_pieces = [group.by_y(*ab, 0) for ab in in_pieces]
    in_full = jnp.concatenate(in_pieces, axis=0)
    out_full = jnp.concatenate(group.ring(group.by_y(*out_pair, 1)), axis=1)
    scales = group.gather_rows(block_scale)
    up_own, up_other = group.trade(columns(ff_gate, ff_up), 0)
    upa, upb = [up_own], [up_other]
    downa, downb = [down_own], [down_other]

    def step(pieces, *after):
        piece = pieces[-1]
        if after:
            piece, *_ = lax.optimization_barrier((piece, *after))
        pieces.append(group.send(piece, group.to_z))

    def apart(a, before):
        return lax.optimization_barrier((a, before))[0]

    step(downa)
    step(upa, in_pieces[0], in_pieces[1])

    normed = rms_norm(whole.astype(F32), gain).astype(BF16)
    gain2 = group.turn(join_x(apart(ffn_gain, normed)))
    normed_c = group.swap_c(normed)
    normed_y = group.swap_y(normed)
    normed_yc = group.swap_c(apart(normed_y, in_pieces[2]))
    normed = jnp.concatenate([normed, normed_y, normed_c, normed_yc], axis=0)
    rows = normed.shape[0]
    positions = jnp.arange(rows, dtype=jnp.int32) % SEQ_LEN
    proj = dot(normed, in_full)
    step(upb, proj)
    k_at, v_at, g_at = heads * DK, 2 * heads * DK, 2 * heads * DK + heads * DV
    qproj, kproj, vproj, gproj = jnp.split(proj, (k_at, v_at, g_at), axis=1)
    query = rotate(qproj.reshape(rows, heads, DK), positions).astype(BF16)
    key = (rotate(kproj.reshape(rows, heads, DK), positions) * DK ** (-0.5)).astype(BF16)
    value = vproj.astype(BF16).reshape(rows, heads, DV)
    rates = lax.dynamic_slice_in_dim(head_rates, (group.y * 2 + group.c) * heads, heads)
    normret = retain(query, key, value, rates, scales)
    gated = (normret * jax.nn.silu(gproj)).astype(BF16)
    step(upa, query, key)
    step(upb)
    for _ in range(2, nz):
        step(upa)
        step(upb)
    step(downb, gated)
    step(downa, gated)

    resid, resid_y = [], []
    for half, (w, t) in enumerate(
        zip(jnp.split(out_full, 2, axis=1), jnp.split(whole, 2, axis=1), strict=True)
    ):
        part = dot(gated, w)
        keep, give = jnp.split(part, 2, axis=0)
        pair = group.swap_c(give.astype(BF16)).astype(F32)
        keep = apart(keep, last_pair) if half else keep
        last_pair = pair = keep + pair
        keep, give = jnp.split(pair, 2, axis=0)
        mine = group.swap_y(give.astype(BF16)).astype(F32)
        keep = apart(keep, last_mine) if half else keep
        last_mine = mine = (keep + mine).astype(BF16)
        t = apart(t, last_now) if half else t
        other = swap_x(mine)
        last_now = now = (t.astype(F32) + (mine.astype(F32) + other.astype(F32))).astype(BF16)
        resid.append(now)
        resid_y.append(group.swap_y(now))
    resid = jnp.concatenate(resid, axis=1)
    normed2 = rms_norm(resid.astype(F32), gain2).astype(BF16)
    normed2_c = group.swap_c(normed2)
    resid_y = jnp.concatenate(resid_y, axis=1)
    normed2_y = rms_norm(apart(resid_y, normed2).astype(F32), gain2).astype(BF16)
    normed2_yc = group.swap_c(normed2_y)
    normed2 = jnp.concatenate([normed2, normed2_y], axis=0)
    normed2_c = jnp.concatenate([normed2_c, normed2_yc], axis=0)

    up_full = group.assemble(upa, upb, gated)

    def hidden_of(a):
        gate_part, up_part = jnp.split(dot(a, up_full), 2, axis=1)
        return (jax.nn.silu(gate_part) * up_part).astype(BF16)

    hidden = hidden_of(normed2)
    step(downb, hidden)
    hidden_c = hidden_of(normed2_c)
    for _ in range(3, nz):
        step(downa, hidden_c)
        step(downb)

    total = []
    squares = 0.0
    for i, now in enumerate(jnp.split(resid, nz, axis=1)):
        weight = group.by_y(downa[i], downb[i], 1)
        halves = dot(hidden, weight), dot(hidden_c, weight)
        part = group.scatter_pair(*halves)
        now = now.astype(F32) + sum_x(part)
        squares += jnp.sum(now * now, axis=-1, keepdims=True)
        total.append(now)
    scale = lax.rsqrt(squares / (tokens.shape[1] * lax.axis_size("tp")) + EPS)
    mine = [
        lax.select_n((group.z - (x * (nz // 2) + k)) % nz, *total) for k in range(nz // 2)
    ]
    return (jnp.concatenate(mine, axis=1) * scale * final_gain.astype(F32)).astype(BF16)


def grouped(fs, tp, heads_here, hidden_here):
    split = fs % 4 == 0 and heads_here % 4 == 0 and hidden_here % 64 == 0
    return split and tp == 2 and fs // 4 == 4


def solution(mesh):
    fs, tp = mesh.shape["fs"], mesh.shape["tp"]

    def body(*args):
        if not grouped(fs, tp, args[7].shape[0], args[10].shape[1]):
            return plain_body(*args)
        return group_body(*args)

    return jax.shard_map(
        body,
        mesh=mesh,
        in_specs=(
            P("fs", "tp"),
            P("tp"),
            P("fs", "tp"),
            P("fs", "tp"),
            P("fs", "tp"),
            P("fs", "tp"),
            P("tp", "fs"),
            P("tp"),
            P("fs"),
            P("tp"),
            P("fs", "tp"),
            P("fs", "tp"),
            P("tp", "fs"),
            P("tp"),
        ),
        out_specs=P("fs", "tp"),
        check_vma=False,
    )
```
